256 devices in a mesh: sp: 64 (over z, y, core), tp: 4 (over x).
Axes of the slice: x: 4, y: 4, z: 8, core: 2. Of those that a mesh axis runs over, the one named last changes fastest.
Arguments:
- residual: bfloat16 [4, 6144, 2048], P('tp', 'sp'), may hold values from -3 to 3
- query_nope: bfloat16 [4, 6144, 1024], P('tp', 'sp'), may hold values from -9 to 9
- query_rope: bfloat16 [4, 6144, 512], P('tp', 'sp'), may hold values from -48 to 48
- latent: bfloat16 [4, 6144, 128], P('tp', 'sp'), may hold values from -6 to 6
- rope_key: bfloat16 [4, 6144, 32], P('tp', 'sp'), may hold values from -48 to 48
- latent_gain: float32 [128], replicated, may hold values from 0.1 to 1.9
- up_key: bfloat16 [128, 1024], replicated, may hold values from -1 to 1
- up_value: bfloat16 [128, 1024], replicated, may hold values from -0.5 to 0.5
- out_weight: bfloat16 [1024, 2048], replicated, may hold values from -0.375 to 0.375
- ffn_gain: float32 [2048], replicated, may hold values from 0.1 to 1.9
- routes: int32 [4, 6144, 2], P(None, 'sp'), may hold values from 0 to 63, all different within a row; in each aligned block of 96 rows (0 to 95, 96 to 191, ..., all dimensions but the last counted through in order) at most 3 rows name the same one
- route_weight: float32 [4, 6144, 2], P('tp', 'sp'), may hold values from 0.1 to 1
- gate_weight: bfloat16 [64, 2048, 1024], P('sp', None, 'tp'), may hold values from -1.5 to 1.5
- up_weight: bfloat16 [64, 2048, 1024], P('sp', None, 'tp'), may hold values from -1.5 to 1.5
- down_weight: bfloat16 [64, 1024, 2048], P('sp', 'tp'), may hold values from -0.046875 to 0.046875
Outputs:
- updated: bfloat16 [4, 6144, 2048], P('tp', 'sp')
The draws below stay inside these ranges and needn't reach their ends.
Inputs may be any that keep to these rules, and one draw needn't show every extreme that they name: `routes`: each row names 2 different experts. In each aligned block of 96 rows (one sequence's rows of one device) no expert is named by more than 3 rows, a bound that some block reaches.
All inputs are finite; a program needn't handle non-finite values.
Results may differ from the reference program's by a relative error of at most 0.017.
Values may be sent and summed in bfloat16 or wider, within the bound.
No kernel may reach another device: no remote copies, remote signals or barrier semaphores. Data moves between devices by JAX's collectives and lax.ppermute only.
A program may use at most 64 MiB of HBM per device.

```python
import math
import jax
import jax.numpy as jnp
import numpy as np
from jax import lax

D = 2048
HEADS = 16
NOPE = 64
ROPE = 32
VDIM = 64
LATENT = 128
FF = 1024
TOPK = 2
TOK_DEV = 96
SEQS = 4
LENGTH = 6144
EXPERTS = 64
FF_BLOCK = 256
MOST = 3
N_SP = 64
N_TP = 4


def rope_pair(key):
    base = jax.random.fold_in(key, 7)
    shape_keys = (SEQS, LENGTH, ROPE)
    shape_queries = (SEQS, LENGTH, HEADS, ROPE)
    keys = jax.random.normal(jax.random.fold_in(base, 1), shape_keys, jnp.float32) * 1.5
    queries = jax.random.normal(jax.random.fold_in(base, 2), shape_queries, jnp.float32) * 1.5
    return (keys, queries.reshape(SEQS, LENGTH, HEADS * ROPE))


def expert_matrix(key, salt):
    base = jax.random.fold_in(key, salt)
    values = jax.random.normal(jax.random.fold_in(base, 1), (EXPERTS, D, FF), jnp.float32)
    columns = jnp.exp(jax.random.uniform(jax.random.fold_in(base, 2), (EXPERTS, 1, FF), jnp.float32, math.log(0.5), math.log(6.0)))
    return jnp.clip(values * columns * D ** (-0.5), -1.5, 1.5)


def draw_query_rope(key, part):
    return rope_pair(key)[1].astype(jnp.bfloat16)


def draw_rope_key(key, part):
    return rope_pair(key)[0].astype(jnp.bfloat16)


def draw_gate_weight(key, part):
    return expert_matrix(key, 101).astype(jnp.bfloat16)


def draw_up_weight(key, part):
    return expert_matrix(key, 202).astype(jnp.bfloat16)


def level_of(stream_key, shape, shards, low, high):
    level, own = 1.0, jax.random.fold_in(stream_key, 6)
    for dim, shards_of in shards:
        steps = jnp.exp(jax.random.uniform(jax.random.fold_in(own, dim), (shards_of,), jnp.float32, low / len(shards), high / len(shards)))
        level = level * jnp.repeat(steps, shape[dim] // shards_of).reshape([-1 if axis == dim else 1 for axis in range(len(shape))])
    return level


def shared_out(own_key, own, number, rows, amount, top, limit, lean):
    order = jax.random.permutation(own_key, amount)
    packed, ordinary = load_shares(amount, rows * top, limit, lean, True), load_shares(amount, rows * top, limit, lean, False)
    places = jnp.arange(amount)

    def named(tallies, offset_by):
        used = int((tallies > 0).sum())
        fixed = max(1, used // 4)
        passed = fixed + (places - fixed + offset_by * (used - fixed)) % max(1, amount - fixed)
        return jnp.zeros((amount,), jnp.int32).at[order[jnp.where(places < fixed, places, passed)]].set(jnp.asarray(tallies, jnp.int32))

    tallies = jnp.where(number % 4 == 0, named(packed, number // 4), named(ordinary, number - number // 4 - 1))
    mixed = jax.random.permutation(jax.random.fold_in(own, 3), amount)
    giver, sink = mixed[0:amount // 2 * 2:2], mixed[1:amount // 2 * 2:2]
    room = jnp.minimum(tallies[giver] - 1, limit - tallies[sink]) // 2
    room = jnp.where((giver == order[0]) | (sink == order[0]) | (tallies[sink] == 0), 0, jnp.maximum(room, 0))
    passed = jax.random.randint(jax.random.fold_in(own, 4), (amount // 2,), 0, 1 << 20) % (room + 1)
    tallies = tallies.at[giver].add(-passed).at[sink].add(passed)
    members = jnp.searchsorted(jnp.cumsum(tallies), jnp.arange(rows * top), side="right").astype(jnp.int32)
    grid = members.reshape(top, rows).T
    grid = grid[jax.random.permutation(jax.random.fold_in(own, 1), rows)]
    offset_by = jax.random.randint(jax.random.fold_in(own, 2), (rows, 1), 0, top)
    return jnp.take_along_axis(grid, (jnp.arange(top)[None, :] + offset_by) % top, axis=1)


def load_shares(count, total, reach, skew, full):
    portions = [(1 << 20) // math.isqrt(standing ** skew) + 1 for standing in range(1, count + 1)]
    largest = reach if full else min(reach, max(-(-total // count), total * portions[0] // sum(portions)))
    least = 1 if total - largest >= count - 1 else 0
    given, rest = [largest] + [least] * (count - 1), total - largest - least * (count - 1)
    while rest > 0:
        candidates = [i for i in range(1, count) if given[i] < largest] or [i for i in range(1, count) if given[i] < reach]
        whole, budget = sum([portions[i] for i in candidates]), rest
        for i in candidates:
            addition = min(reach - given[i], max(1, budget * portions[i] // whole), rest)
            given[i] = given[i] + addition
            rest = rest - addition
    return np.array(given)


def bell_draw(own_key, dims, spread, most, shards=(), held_as=jnp.bfloat16):
    loudness = level_of(own_key, dims, shards, -0.22, 0.18) if shards else 1.0
    values = jax.random.normal(own_key, dims, jnp.float32) * spread * loudness
    return jnp.minimum(jnp.maximum(values, -most), most).astype(held_as)


def setup_inputs(seed: int = 0) -> dict:
    key_list = jax.random.split(jax.random.key(seed), 16)
    residual = bell_draw(key_list[0], (SEQS, LENGTH, D), 0.5, 3.0, ((0, 4), (1, 64)))
    query_nope = bell_draw(key_list[1], (SEQS, LENGTH, HEADS * NOPE), 1.5, 9.0, ((0, 4), (1, 64)))
    query_rope = draw_query_rope(jax.random.fold_in(key_list[15], 71), 0)
    latent = bell_draw(key_list[3], (SEQS, LENGTH, LATENT), 1.0, 6.0, ((0, 4), (1, 64)))
    rope_key = draw_rope_key(jax.random.fold_in(key_list[15], 71), 0)
    latent_gain = jnp.clip(1.0 + 0.18 * jax.random.normal(key_list[5], (LATENT,), jnp.float32), 0.1, 1.9)
    up_key = bell_draw(key_list[6], (LATENT, HEADS * NOPE), (LATENT // 3) ** -0.5, 1.0)
    up_value = bell_draw(key_list[7], (LATENT, HEADS * VDIM), LATENT ** -0.5, 0.5)
    out_weight = bell_draw(key_list[8], (HEADS * VDIM, D), (HEADS * VDIM // 4) ** -0.5, 0.375)
    ffn_gain = jnp.clip(1.0 + 0.18 * jax.random.normal(key_list[9], (D,), jnp.float32), 0.1, 1.9)
    routes_keys = jax.random.split(jax.random.fold_in(key_list[10], 1), SEQS * LENGTH // TOK_DEV)
    routes_turns = jax.random.permutation(jax.random.fold_in(key_list[10], 3), SEQS * LENGTH // TOK_DEV)
    routes = jax.vmap(lambda own, number: shared_out(jax.random.fold_in(key_list[10], 2), own, number, TOK_DEV, EXPERTS, TOPK, MOST, 0))(routes_keys, routes_turns).reshape((SEQS, LENGTH, TOPK))
    route_weight = jnp.clip(jnp.exp(math.log(1.0) - 2.3025851 * jax.random.uniform(key_list[11], (SEQS, LENGTH, TOPK), jnp.float32) ** level_of(key_list[11], (SEQS, LENGTH, TOPK), ((0, 4), (1, 64)), -0.2, 0.2)), 0.1, 1.0)
    gate_weight = draw_gate_weight(jax.random.fold_in(key_list[15], 71), 0)
    up_weight = draw_up_weight(jax.random.fold_in(key_list[15], 71), 0)
    down_weight = bell_draw(key_list[14], (EXPERTS, FF, D), (FF * 16) ** -0.5, 0.046875, ((0, 64), (1, 4)))
    return dict(residual=residual, query_nope=query_nope, query_rope=query_rope, latent=latent, rope_key=rope_key, latent_gain=latent_gain, up_key=up_key, up_value=up_value, out_weight=out_weight, ffn_gain=ffn_gain, routes=routes, route_weight=route_weight, gate_weight=gate_weight, up_weight=up_weight, down_weight=down_weight)


EPS = 1e-06
ROPE_BASE = 10000.0
CLAMP = 7.0
ALPHA = 1.702

def rotate(values, positions, width):
    half = width // 2
    inverse = ROPE_BASE ** (-jnp.arange(half, dtype=jnp.float32) * 2.0 / width)
    angle = positions.astype(jnp.float32)[:, None] * inverse[None, :]
    cosine = jnp.cos(angle)[:, None, :]
    sine = jnp.sin(angle)[:, None, :]
    first = values[..., :half]
    second = values[..., half:]
    return jnp.concatenate([first * cosine - second * sine, first * sine + second * cosine], axis=-1)

def rms_scaled(values, gain):
    return values * lax.rsqrt(lax.optimization_barrier(jnp.mean(values * values, axis=-1, keepdims=True)) + EPS) * gain

def reference(residual, query_nope, query_rope, latent, rope_key, latent_gain, up_key, up_value, out_weight, ffn_gain, routes, route_weight, gate_weight, up_weight, down_weight):
    sequences, length, width = residual.shape
    positions = jnp.arange(length, dtype=jnp.int32)
    factor = (NOPE + ROPE) ** (-0.5)
    normed = rms_scaled(latent.astype(jnp.float32), latent_gain).astype(jnp.bfloat16)
    flat_latent = normed.reshape(-1, LATENT)
    key_part = jnp.dot(flat_latent, up_key, preferred_element_type=jnp.float32).astype(jnp.bfloat16)
    key_part = key_part.reshape(sequences, length, HEADS, NOPE)
    value_part = jnp.dot(flat_latent, up_value, preferred_element_type=jnp.float32).astype(jnp.bfloat16)
    value_part = value_part.reshape(sequences, length, HEADS, VDIM)
    key_turned = rotate(rope_key.astype(jnp.float32)[:, :, None, :], positions, ROPE)[:, :, 0, :].astype(jnp.bfloat16)
    query_turned = rotate(query_rope.astype(jnp.float32).reshape(sequences, length, HEADS, ROPE), positions, ROPE).astype(jnp.bfloat16)
    query_plain = query_nope.reshape(sequences, length, HEADS, NOPE)
    span = math.gcd(length, 256)
    count = length // span

    def one_sequence(items):
        plain, turned, keys, turned_keys, values = items
        keys_wide = keys.astype(jnp.float32)
        turned_wide = turned_keys.astype(jnp.float32)
        values_wide = values.astype(jnp.float32)

        def one_block(pair):
            scores = (jnp.einsum('qhd,khd->hqk', pair[0].astype(jnp.float32), keys_wide) + jnp.einsum('qhd,kd->hqk', pair[1].astype(jnp.float32), turned_wide)) * factor
            peak = lax.optimization_barrier(jnp.max(scores, axis=-1, keepdims=True))
            weights = jnp.exp(scores - peak)
            total = lax.optimization_barrier(jnp.sum(weights, axis=-1))
            rounded = lax.optimization_barrier(weights.astype(jnp.bfloat16)).astype(jnp.float32)
            mixed = jnp.einsum('hqk,khd->qhd', rounded, values_wide)
            return (mixed / jnp.transpose(total)[:, :, None]).astype(jnp.bfloat16)
        blocks = lax.map(one_block, (plain.reshape(count, span, HEADS, NOPE), turned.reshape(count, span, HEADS, ROPE)))
        return blocks.reshape(length, HEADS * VDIM)
    attended = lax.map(one_sequence, (query_plain, query_turned, key_part, key_turned, value_part))
    projected = jnp.dot(attended.reshape(-1, HEADS * VDIM), out_weight, preferred_element_type=jnp.float32)
    middle = (residual.reshape(-1, width).astype(jnp.float32) + projected).astype(jnp.bfloat16)
    middle_wide = lax.optimization_barrier(middle).astype(jnp.float32)
    normal_rows = rms_scaled(middle_wide, ffn_gain).astype(jnp.bfloat16)
    total_rows = sequences * length
    flat_picks = routes.reshape(-1)
    flat_weights = route_weight.reshape(-1)
    owner = jnp.arange(total_rows * TOPK, dtype=jnp.int32) // TOPK
    capacity = sequences * N_SP * MOST
    padded = jnp.concatenate([normal_rows, jnp.zeros((1, width), jnp.bfloat16)], axis=0)

    def one_expert(accum, items):
        gate_w, up_w, down_w, index = items
        hit = flat_picks == index
        rank = jnp.cumsum(hit.astype(jnp.int32)) - 1
        slot = jnp.where(hit, rank, capacity).astype(jnp.int32)
        source = jnp.full((capacity + 1,), total_rows, jnp.int32).at[slot].set(owner)[:capacity]
        scale_rows = jnp.zeros((capacity + 1,), jnp.float32).at[slot].set(flat_weights)[:capacity]
        rows = padded[source]
        gate = jnp.minimum(jnp.dot(rows, gate_w, preferred_element_type=jnp.float32), CLAMP)
        lift = jnp.clip(jnp.dot(rows, up_w, preferred_element_type=jnp.float32), -CLAMP, CLAMP)
        active = (gate * jax.nn.sigmoid(ALPHA * gate) * (lift + 1.0)).astype(jnp.bfloat16)
        parts = jnp.einsum('rjf,jfd->jrd', active.reshape(capacity, N_TP, FF_BLOCK).astype(jnp.float32), down_w.reshape(N_TP, FF_BLOCK, width).astype(jnp.float32))
        output = lax.optimization_barrier(jnp.sum(lax.optimization_barrier(parts.astype(jnp.bfloat16)).astype(jnp.float32), axis=0))
        output = output.astype(jnp.bfloat16)
        accum = accum.at[source].add(output.astype(jnp.float32) * scale_rows[:, None])
        return (accum, None)
    accum, _ = lax.scan(one_expert, jnp.zeros((total_rows + 1, width), jnp.float32), (gate_weight, up_weight, down_weight, jnp.arange(EXPERTS, dtype=jnp.int32)))
    updated = (middle_wide + accum[:total_rows]).astype(jnp.bfloat16)
    return updated.reshape(sequences, length, width)
```

```python
import math

import jax
import jax.numpy as jnp
from jax import lax
from jax.experimental import pallas as pl
from jax.experimental.pallas import tpu as pltpu
from jax.sharding import Mesh
from jax.sharding import PartitionSpec as P

D = 2048
HEADS = 16
NOPE = 64
ROPE = 32
LATENT = 128
TOK = 96
EXPERTS = 64
SLOTS = 3
SP = ("sp_0", "sp_1", "sp_2")
N_Z, N_Y, N_C, N_X = 8, 4, 2, 4

EPS = 1e-06
ROPE_BASE = 10000.0
CLAMP = 7.0
ALPHA = 1.702
NEG_BIG = -1e30
SCALE = (NOPE + ROPE) ** (-0.5) * math.log2(math.e)

ROWS = HEADS * TOK
Q_TILE = 768
GROUPS = TOK // ROPE
KEYS = 1024
CHUNKS = 2 * GROUPS
PAIRS = HEADS // 2
BLOCK = SLOTS * D // 128
COLS = D // 128


def ring(n, d):
    return [(i, (i + d) % n) for i in range(n)]


def contract(a, b, dims):
    return lax.dot_general(a, b, (dims, ((), ())), preferred_element_type=jnp.float32)


def iota(shape, dim):
    return lax.broadcasted_iota(jnp.int32, shape, dim)


def vmem():
    return pl.BlockSpec(memory_space=pltpu.VMEM)


def call(kernel, outs, scratch, n_in, flops, name, limit):
    return pl.pallas_call(
        kernel,
        out_shape=outs,
        in_specs=[vmem()] * n_in,
        out_specs=jax.tree.map(lambda _: vmem(), outs),
        scratch_shapes=scratch,
        compiler_params=pltpu.CompilerParams(vmem_limit_bytes=limit << 20),
        cost_estimate=pl.CostEstimate(flops=flops, bytes_accessed=1 << 20, transcendentals=0),
        name=name,
    )


def pack_kernel(latent, gain, rope, cos, sin, out):
    wide = latent[...].astype(jnp.float32)
    normed = wide * lax.rsqrt(jnp.mean(wide * wide, axis=-1, keepdims=True) + EPS) * gain[...]
    src, dst = iota((ROPE, 128), 0), iota((ROPE, 128), 1)
    plain = jnp.zeros((ROPE, 128), jnp.float32)
    other = jnp.zeros((ROPE, 128), jnp.float32)
    swapped = (src + ROPE // 2) % ROPE
    for g in range(GROUPS):
        part = rope[ROPE * g : ROPE * (g + 1), :]
        plain += contract(part, (dst == src + ROPE * g).astype(jnp.bfloat16), ((1,), (0,)))
        other += contract(part, (dst == swapped + ROPE * g).astype(jnp.bfloat16), ((1,), (0,)))
    turned = plain * cos[...] + other * sin[...]
    packed = jnp.concatenate([normed, turned], axis=0).astype(jnp.bfloat16)
    for k in range(N_Z):
        out[k] = packed


def slot_hits(routes, pick):
    slot = iota((SLOTS * EXPERTS, TOK), 0)
    return routes[pick : pick + 1, :] == slot % EXPERTS


def slot_match(routes):
    hits = [slot_hits(routes, k) for k in range(2)]
    either = jnp.where(hits[0] | hits[1], 1.0, 0.0)
    earlier = (iota((TOK, TOK), 0) < iota((TOK, TOK), 1)).astype(jnp.float32).astype(jnp.bfloat16)
    rank = contract(either.astype(jnp.bfloat16), earlier, ((1,), (0,)))
    wanted = (iota((SLOTS * EXPERTS, TOK), 0) // EXPERTS).astype(jnp.float32)
    return [h & (rank == wanted) for h in hits]


def spread(rows, wide, out):
    for c in range(COLS):
        for r in range(SLOTS):
            wide[pl.ds(c * SLOTS + r, EXPERTS, stride=BLOCK), :] = rows[
                r * EXPERTS : (r + 1) * EXPERTS, 128 * c : 128 * (c + 1)
            ]
    out[...] = wide[...].astype(jnp.bfloat16)


def collect(wide, c):
    parts = [wide[pl.ds(c * SLOTS + r, EXPERTS, stride=BLOCK), :] for r in range(SLOTS)]
    return jnp.concatenate(parts, axis=0).astype(jnp.bfloat16)


def attend_kernel(
    kv0, kv1, qn, qr, uk, uv, cos, sin, res, ow, fg, routes, mid_o, out_o, qs, ks, acc, peak, wide
):
    lane = iota((TOK, 128), 1)
    for j in range(PAIRS):
        x = qn[:, 128 * j : 128 * (j + 1)].astype(jnp.float32)
        u = uk[:, 128 * j : 128 * (j + 1)]
        for k in range(2):
            one = jnp.where(lane // NOPE == k, x, 0.0).astype(jnp.bfloat16)
            q = (contract(one, u, ((1,), (1,))) * SCALE).astype(jnp.bfloat16)
            for g in range(GROUPS):
                qs[g, pl.ds((2 * j + k) * TOK, TOK), 0:128] = q
    for j in range(HEADS // 4):
        x = qr[:, 128 * j : 128 * (j + 1)].astype(jnp.float32)
        half = ROPE // 2
        other = jnp.where(lane % ROPE < half, pltpu.roll(x, 128 - half, 1), pltpu.roll(x, half, 1))
        turned = (x * cos[...] + other * sin[...]) * SCALE
        for k in range(4):
            for g in range(GROUPS):
                shift = (ROPE * (g - k)) % 128
                moved = turned if shift == 0 else pltpu.roll(turned, shift, 1)
                kept = jnp.where(lane // ROPE == g, moved, 0.0).astype(jnp.bfloat16)
                qs[g, pl.ds((4 * j + k) * TOK, TOK), 128:256] = kept
    for h, kv in enumerate((kv0, kv1)):
        turned = kv[:, TOK : TOK + ROPE, :].reshape(KEYS, 128)
        for g in range(GROUPS):
            ks[h * GROUPS + g, :, 0:128] = kv[:, ROPE * g : ROPE * (g + 1), :].reshape(KEYS, 128)
            ks[h * GROUPS + g, :, 128:256] = turned
    acc[...] = jnp.zeros_like(acc)
    peak[...] = jnp.full_like(peak, NEG_BIG)

    def step(i, _):
        chunk = i // (ROWS // Q_TILE)
        at = pl.ds(pl.multiple_of(i % (ROWS // Q_TILE) * Q_TILE, Q_TILE), Q_TILE)
        keys = ks[chunk]
        scores = contract(qs[chunk % GROUPS, at, :], keys, ((1,), (1,)))
        old = peak[at, :]
        new = jnp.maximum(old, jnp.max(scores, axis=-1, keepdims=True))
        weights = jnp.exp2(scores - new[:, 0:1]).astype(jnp.bfloat16)
        values = jnp.concatenate([keys[:, 0:128], jnp.ones((KEYS, 128), jnp.bfloat16)], axis=1)
        mixed = contract(weights, values, ((1,), (0,)))
        shrink = jnp.exp2(old - new)
        acc[at, :] = acc[at, :] * jnp.concatenate([shrink, shrink], axis=1) + mixed
        peak[at, :] = new
        return 0

    lax.fori_loop(0, CHUNKS * (ROWS // Q_TILE), step, 0)

    lane2 = iota((LATENT, 128), 1)
    heads = []
    for j in range(PAIRS):
        pair = []
        for k in range(2):
            at = pl.ds((2 * j + k) * TOK, TOK)
            pair.append((acc[at, 0:128] / acc[at, 128:256]).astype(jnp.bfloat16))
        u = uv[:, 128 * j : 128 * (j + 1)].astype(jnp.float32)
        both = jnp.concatenate(
            [jnp.where(lane2 // NOPE == k, u, 0.0).astype(jnp.bfloat16) for k in range(2)], axis=0
        )
        heads.append(
            contract(jnp.concatenate(pair, axis=1), both, ((1,), (0,))).astype(jnp.bfloat16)
        )
    projected = contract(jnp.concatenate(heads, axis=1), ow[...], ((1,), (0,)))
    middle = (res[...].astype(jnp.float32) + projected).astype(jnp.bfloat16)
    mid_o[...] = middle
    mid = middle.astype(jnp.float32)
    normal = mid * lax.rsqrt(jnp.mean(mid * mid, axis=-1, keepdims=True) + EPS) * fg[...]
    first, second = slot_match(routes)
    chosen = jnp.where(first | second, 1.0, 0.0).astype(jnp.bfloat16)
    spread(contract(chosen, normal.astype(jnp.bfloat16), ((1,), (0,))), wide, out_o)


def gated(gate, lift):
    gate = jnp.minimum(gate, CLAMP)
    lift = jnp.clip(lift, -CLAMP, CLAMP)
    return (gate * jax.nn.sigmoid(ALPHA * gate) * (lift + 1.0)).astype(jnp.bfloat16)


def expert_kernel(arrived, g0, u0, d0, g1, u1, d1, g2, u2, d2, ga, gb, ua, ub, da, db, out, x, wide):
    wide[...] = arrived[...].astype(jnp.float32)
    for c in range(COLS):
        x[:, 128 * c : 128 * (c + 1)] = collect(wide, c)
    total = None
    for g, u, d in ((g0, u0, d0), (g1, u1, d1), (g2, u2, d2)):
        rows = x[...]
        a = gated(contract(rows, g[...], ((1,), (0,))), contract(rows, u[...], ((1,), (0,))))
        term = contract(a, d[...], ((1,), (0,)))
        total = term if total is None else total + term
    n = ga.shape[0]
    left, right = x[:, :n], x[:, n:]
    a = gated(
        contract(left, ga[...], ((1,), (0,))) + contract(right, gb[...], ((1,), (0,))),
        contract(left, ua[...], ((1,), (0,))) + contract(right, ub[...], ((1,), (0,))),
    )
    m = da.shape[0]
    total += contract(a[:, :m], da[...], ((1,), (0,))) + contract(a[:, m:], db[...], ((1,), (0,)))
    total = total.astype(jnp.bfloat16).astype(jnp.float32)
    spread(total, wide, out)


def combine_kernel(returned, mid, routes, weight, out, wide):
    wide[...] = returned[...].astype(jnp.float32)
    share = 0.0
    for k, m in enumerate(slot_match(routes)):
        share += jnp.where(m, weight[k : k + 1, :], 0.0)
    high = share.astype(jnp.bfloat16)
    low = (share - high.astype(jnp.float32)).astype(jnp.bfloat16)
    for c in range(COLS):
        rows = collect(wide, c)
        added = contract(high, rows, ((0,), (0,))) + contract(low, rows, ((0,), (0,)))
        at = slice(128 * c, 128 * (c + 1))
        out[:, at] = (mid[:, at].astype(jnp.float32) + added).astype(jnp.bfloat16)


def angles(positions, shape):
    inverse = ROPE_BASE ** (-jnp.arange(ROPE // 2, dtype=jnp.float32) * 2.0 / ROPE)
    lane = jnp.arange(128, dtype=jnp.int32)
    angle = positions.astype(jnp.float32) * inverse[lane % (ROPE // 2)][None, :]
    sign = jnp.where(lane % ROPE < ROPE // 2, -1.0, 1.0).astype(jnp.float32)
    return jnp.cos(angle), jnp.sin(angle) * sign[None, :]


def sent_half(blocks):
    ahead, behind = blocks
    half = ahead.shape[0] // 2
    return (
        lax.ppermute(ahead[:half], "tp", ring(N_X, 1)),
        lax.ppermute(behind[half:], "tp", ring(N_X, N_X - 1)),
    )


def local(
    residual,
    query_nope,
    query_rope,
    latent,
    rope_key,
    latent_gain,
    up_key,
    up_value,
    out_weight,
    ffn_gain,
    routes,
    route_weight,
    gate_weight,
    up_weight,
    down_weight,
):
    bf, f32 = jnp.bfloat16, jnp.float32
    weights = (gate_weight[0], up_weight[0], down_weight[0])
    near = [
        (lax.ppermute(w, "tp", ring(N_X, 1)), lax.ppermute(w, "tp", ring(N_X, N_X - 1)))
        for w in weights
    ]

    base = lax.axis_index(SP) * TOK
    lane = jnp.arange(128, dtype=jnp.int32)[None, :]
    cos_q, sin_q = angles(base + jnp.arange(TOK, dtype=jnp.int32)[:, None], None)
    row = jnp.arange(ROPE, dtype=jnp.int32)[:, None]
    cos_k, sin_k = angles(base + row + lane // ROPE * ROPE, None)
    own_routes = jnp.transpose(
        lax.dynamic_index_in_dim(routes, lax.axis_index("tp"), 0, keepdims=False)
    )
    own_weight = jnp.transpose(route_weight[0])

    packed = call(
        pack_kernel, jax.ShapeDtypeStruct((N_Z, 128, 128), bf), [], 5, 1 << 22, "pack", 16
    )(latent[0], latent_gain[None], rope_key[0], cos_k, sin_k)
    line = lax.all_to_all(packed, "sp_0", 0, 0, tiled=True).reshape(N_Z * 128, 128)
    plane = lax.all_to_all(
        jnp.broadcast_to(line[None], (N_Y, N_Z * 128, 128)), "sp_1", 0, 0, tiled=True
    ).reshape(N_Y * N_Z, 128, 128)
    other = lax.ppermute(plane, "sp_2", ring(N_C, 1))

    middle, outgoing = call(
        attend_kernel,
        (
            jax.ShapeDtypeStruct((TOK, D), bf),
            jax.ShapeDtypeStruct((EXPERTS * BLOCK, 128), bf),
        ),
        [
            pltpu.VMEM((GROUPS, ROWS, 256), bf),
            pltpu.VMEM((CHUNKS, KEYS, 256), bf),
            pltpu.VMEM((ROWS, 256), f32),
            pltpu.VMEM((ROWS, 128), f32),
            pltpu.VMEM((EXPERTS * BLOCK, 128), f32),
        ],
        12,
        1 << 33,
        "attend",
        44,
    )(
        plane,
        other,
        query_nope[0],
        query_rope[0],
        up_key,
        up_value,
        cos_q,
        sin_q,
        residual[0],
        out_weight,
        ffn_gain[None],
        own_routes,
    )
    near, outgoing = lax.optimization_barrier((near, outgoing))
    far = [sent_half(blocks) for blocks in near]
    arrived = lax.all_to_all(
        outgoing.reshape(EXPERTS, BLOCK, 128), SP, 0, 0, tiled=True
    ).reshape(EXPERTS * BLOCK, 128)
    made = call(
        expert_kernel,
        jax.ShapeDtypeStruct((EXPERTS * BLOCK, 128), bf),
        [pltpu.VMEM((SLOTS * EXPERTS, D), bf), pltpu.VMEM((EXPERTS * BLOCK, 128), f32)],
        16,
        1 << 32,
        "experts",
        40,
    )(
        arrived,
        *weights,
        *[blocks[0] for blocks in near],
        *[blocks[1] for blocks in near],
        *[half for blocks in far for half in blocks],
    )
    returned = lax.all_to_all(
        made.reshape(EXPERTS, BLOCK, 128), SP, 0, 0, tiled=True
    ).reshape(EXPERTS * BLOCK, 128)
    updated = call(
        combine_kernel,
        jax.ShapeDtypeStruct((TOK, D), bf),
        [pltpu.VMEM((EXPERTS * BLOCK, 128), f32)],
        4,
        1 << 28,
        "combine",
        24,
    )(returned, middle, own_routes, own_weight)
    return updated[None]


def solution(mesh):
    split = Mesh(
        mesh.devices.reshape(N_Z, N_Y, N_C, mesh.shape["tp"]), ("sp_0", "sp_1", "sp_2", "tp")
    )
    in_specs = (
        P("tp", SP, None),
        P("tp", SP, None),
        P("tp", SP, None),
        P("tp", SP, None),
        P("tp", SP, None),
        P(),
        P(),
        P(),
        P(),
        P(),
        P(None, SP, None),
        P("tp", SP, None),
        P(SP, None, "tp"),
        P(SP, None, "tp"),
        P(SP, "tp", None),
    )
    out_specs = P("tp", SP, None)
    return jax.shard_map(local, mesh=split, in_specs=in_specs, out_specs=out_specs, check_vma=False)
```
